32 devices in a mesh: grp: 2 (over y), fs: 4 (over z), tp: 4 (over x, core).
Axes of the slice: x: 2, y: 2, z: 4, core: 2. Of those that a mesh axis runs over, the one named last changes fastest.
Arguments:
- tokens: bfloat16 [4096, 2048], P(('grp', 'fs'), 'tp'), parts along dimension 0, may hold values from -16 to 16
- attn_gain: float32 [2048], replicated, may hold values from 0.1 to 1.9
- w_query: bfloat16 [2048, 1024], P('fs', 'tp'), may hold values from -0.125 to 0.125
- w_key: bfloat16 [2048, 1024], P('fs', 'tp'), may hold values from -0.125 to 0.125
- w_value: bfloat16 [2048, 2048], P('fs', 'tp'), may hold values from -0.125 to 0.125
- w_low: bfloat16 [2048, 32], replicated, may hold values from -0.125 to 0.125
- w_lift: bfloat16 [32, 1024], P(None, 'tp'), may hold values from -1 to 1
- decay_bias: float32 [1024], P('tp'), may hold values from -0.5 to 6
- head_gain: float32 [256], replicated, may hold values from 0.1 to 1.9
- w_out: bfloat16 [2048, 2048], P('tp', 'fs'), may hold values from -0.125 to 0.125
- ffn_gain: float32 [2048], replicated, may hold values from 0.1 to 1.9
- w_gate: bfloat16 [2048, 5632], P('fs', 'tp'), may hold values from -0.125 to 0.125
- w_up: bfloat16 [2048, 5632], P('fs', 'tp'), may hold values from -0.125 to 0.125
- w_down: bfloat16 [5632, 2048], P('tp', 'fs'), may hold values from -0.078125 to 0.078125
- final_gain: float32 [2048], P('tp'), may hold values from 0.1 to 1.9
Outputs:
- result: bfloat16 [4096, 2048], P(('grp', 'fs'), 'tp'), parts along dimension 0
The draws below stay inside these ranges and needn't reach their ends.
There are 2 independent parts, one for each index of `grp`. The reference program is written for one: setup_inputs(seed, part) draws one part's arguments, and reference() takes and returns one part's arrays. A program takes and returns all parts, laid end to end along the dimension named above; an argument that names none is the same for every part. Nothing has to cross between parts.
All inputs are finite; a program needn't handle non-finite values.
Results may differ from the reference program's by a relative error of at most 0.015.
Values may be sent and summed in bfloat16 or wider, within the bound.
A program may use at most 64 MiB of HBM per device.

```python
import math
import jax
import jax.numpy as jnp
from jax import lax

D = 2048
HEADS = 8
DK = 128
DV = 256
RANK = 32
FF = 5632
BLOCK = 64
LEN = 512
QK = 1024
V = 2048
TOKENS = 2048
N_FS = 4
N_TP = 4


def draw_tokens(key, part):
    first_key, second_key = jax.random.split(jax.random.fold_in(key, 11), 2)
    groups = 8
    scales = jnp.exp(jax.random.uniform(first_key, (groups,), jnp.float32, math.log(0.25), math.log(4.0)))
    scales = jnp.repeat(scales, D // groups)
    base = jnp.clip(jax.random.normal(second_key, (TOKENS, D), jnp.float32), -4.0, 4.0)
    return (base * scales[None, :]).astype(jnp.bfloat16)


def draw_decay_bias(key, part):
    first_key, second_key, third_key = jax.random.split(jax.random.fold_in(key, 23), 3)
    fast_share = 0.5
    is_fast = jax.random.uniform(first_key, (QK,), jnp.float32) < fast_share
    fast_value = jax.random.uniform(second_key, (QK,), jnp.float32, -0.5, 0.5)
    slow_value = jax.random.uniform(third_key, (QK,), jnp.float32, 4.5, 6.0)
    return jnp.where(is_fast, fast_value, slow_value)


def block_levels(stream_key, extent, shards, smallest, high):
    def one(axis_at, shards_of):
        heights = jax.random.uniform(jax.random.fold_in(jax.random.fold_in(stream_key, 6), axis_at), (shards_of,), jnp.float32, smallest / len(shards), high / len(shards))
        return jnp.repeat(jnp.exp(heights), extent[axis_at] // shards_of).reshape((-1,) + (1,) * (len(extent) - axis_at - 1))

    level = one(*shards[0])
    for cut in shards[1:]:
        level = level * one(*cut)
    return level


def noise(key, shape, width, bound, pieces=(), kind=jnp.bfloat16):
    values = width * jax.random.normal(key, shape, jnp.float32)
    if pieces:
        values = values * block_levels(key, shape, pieces, -0.22, 0.18)
    return jnp.clip(values, -bound, bound).astype(kind)


def setup_inputs(seed: int = 0, part: int = 0) -> dict:
    streams_of = jax.random.split(jax.random.key(seed), 16)
    own_keys = jax.random.split(jax.random.fold_in(streams_of[15], part), 16)
    return {
        "tokens": draw_tokens(jax.random.fold_in(jax.random.fold_in(streams_of[15], part), 71), part),
        "attn_gain": jnp.clip(1.0 + 0.18 * jax.random.normal(streams_of[1], (D,), jnp.float32), 0.1, 1.9),
        "w_query": noise(streams_of[2], (D, QK), D ** -0.5, 0.125, ((0, 4), (1, 4))),
        "w_key": noise(streams_of[3], (D, QK), D ** -0.5, 0.125, ((0, 4), (1, 4))),
        "w_value": noise(streams_of[4], (D, V), D ** -0.5, 0.125, ((0, 4), (1, 4))),
        "w_low": noise(streams_of[5], (D, RANK), D ** -0.5, 0.125),
        "w_lift": noise(streams_of[6], (RANK, QK), RANK ** -0.5, 1.0, ((1, 4),)),
        "decay_bias": draw_decay_bias(jax.random.fold_in(streams_of[15], 71), part),
        "head_gain": jnp.clip(1.0 + 0.18 * jax.random.normal(streams_of[8], (DV,), jnp.float32), 0.1, 1.9),
        "w_out": noise(streams_of[9], (V, D), V ** -0.5, 0.125, ((0, 4), (1, 4))),
        "ffn_gain": jnp.clip(1.0 + 0.18 * jax.random.normal(streams_of[10], (D,), jnp.float32), 0.1, 1.9),
        "w_gate": noise(streams_of[11], (D, FF), D ** -0.5, 0.125, ((0, 4), (1, 4))),
        "w_up": noise(streams_of[12], (D, FF), D ** -0.5, 0.125, ((0, 4), (1, 4))),
        "w_down": noise(streams_of[13], (FF, D), FF ** -0.5, 0.078125, ((0, 4), (1, 4))),
        "final_gain": jnp.clip(1.0 + 0.18 * jax.random.normal(streams_of[14], (D,), jnp.float32), 0.1, 1.9),
    }


epsilon = 1e-06
highest = lax.Precision.HIGHEST

def rms_rows(values, gain):
    values = values.astype(jnp.float32)
    factor = lax.rsqrt(lax.optimization_barrier(jnp.mean(values * values, axis=-1, keepdims=True)) + epsilon)
    return values * factor * gain.astype(jnp.float32)

def blockwise_gla(query_rows, key_rows, value_rows, log_decay, head_count):
    length = query_rows.shape[0]
    blocks = length // BLOCK

    def split_heads(array, depth):
        return array.astype(jnp.float32).reshape(blocks, BLOCK, head_count, depth).transpose(2, 0, 1, 3)
    query_f = split_heads(query_rows, DK) * DK ** (-0.5)
    key_f = split_heads(key_rows, DK)
    value_f = split_heads(value_rows, DV)
    log_cum = jnp.cumsum(split_heads(log_decay, DK), axis=2)
    log_last = log_cum[:, :, -1:, :]
    query_dec = query_f * jnp.exp(log_cum)
    key_dec = key_f * jnp.exp(-log_cum)
    causal = jnp.tril(jnp.ones((BLOCK, BLOCK), dtype=bool))
    scores = jnp.where(causal, jnp.einsum('hncd,hnsd->hncs', query_dec, key_dec, precision=highest), 0.0)
    inside = jnp.einsum('hncs,hnsv->hncv', scores, value_f, precision=highest)
    contrib = jnp.einsum('hncd,hncv->hndv', key_f * jnp.exp(log_last - log_cum), value_f, precision=highest)
    decay_block = jnp.exp(log_last[:, :, 0, :])

    def advance(carry_state, inputs):
        decay_step, added = inputs
        return (decay_step[..., None] * carry_state + added, carry_state)
    start_state = jnp.zeros((head_count, DK, DV), jnp.float32)
    final_state, earlier = lax.scan(advance, start_state, (jnp.moveaxis(decay_block, 1, 0), jnp.moveaxis(contrib, 1, 0)))
    earlier = jnp.moveaxis(earlier, 0, 1)
    output = inside + jnp.einsum('hncd,hndv->hncv', query_dec, earlier, precision=highest)
    return output.transpose(1, 2, 0, 3).reshape(length, head_count, DV)

def reference(tokens, attn_gain, w_query, w_key, w_value, w_low, w_lift, decay_bias, head_gain, w_out, ffn_gain, w_gate, w_up, w_down, final_gain):
    normed = rms_rows(tokens, attn_gain).astype(jnp.bfloat16)
    query_rows = jnp.dot(normed, w_query, preferred_element_type=jnp.float32).astype(jnp.bfloat16)
    key_rows = jnp.dot(normed, w_key, preferred_element_type=jnp.float32).astype(jnp.bfloat16)
    value_rows = jnp.dot(normed, w_value, preferred_element_type=jnp.float32).astype(jnp.bfloat16)
    low_rank = jnp.dot(normed, w_low, preferred_element_type=jnp.float32).astype(jnp.bfloat16)
    log_decay = jax.nn.log_sigmoid(jnp.dot(low_rank, w_lift, preferred_element_type=jnp.float32) + decay_bias.astype(jnp.float32)) / 16.0
    gla_out = jax.vmap(lambda qq, kk, vv, gg: blockwise_gla(qq, kk, vv, gg, HEADS))(query_rows.reshape(N_FS, LEN, QK), key_rows.reshape(N_FS, LEN, QK), value_rows.reshape(N_FS, LEN, V), log_decay.reshape(N_FS, LEN, QK))
    gla_out = gla_out.reshape(TOKENS, HEADS, DV)
    mixed_heads = rms_rows(gla_out, head_gain).reshape(TOKENS, V).astype(jnp.bfloat16)
    span = V // N_TP
    attn_sum = jnp.zeros((TOKENS, D), jnp.float32)
    for index in range(N_TP):
        partial_prod = jnp.dot(mixed_heads[:, index * span:(index + 1) * span], w_out[index * span:(index + 1) * span], preferred_element_type=jnp.float32).astype(jnp.bfloat16)
        attn_sum = attn_sum + partial_prod.astype(jnp.float32)
    first_sum = (tokens.astype(jnp.float32) + attn_sum).astype(jnp.bfloat16)
    normed_ffn = rms_rows(first_sum, ffn_gain).astype(jnp.bfloat16)
    gate_rows = jnp.dot(normed_ffn, w_gate, preferred_element_type=jnp.float32)
    up_rows = jnp.dot(normed_ffn, w_up, preferred_element_type=jnp.float32)
    hidden = (jax.nn.silu(gate_rows) * up_rows).astype(jnp.bfloat16)
    units = FF // N_TP
    ffn_sum = jnp.zeros((TOKENS, D), jnp.float32)
    for index in range(N_TP):
        partial_prod = jnp.dot(hidden[:, index * units:(index + 1) * units], w_down[index * units:(index + 1) * units], preferred_element_type=jnp.float32).astype(jnp.bfloat16)
        ffn_sum = ffn_sum + partial_prod.astype(jnp.float32)
    second_sum = first_sum.astype(jnp.float32) + ffn_sum
    return rms_rows(second_sum, final_gain).astype(jnp.bfloat16)
```

```python
import functools

import jax
import jax.numpy as jnp
from jax import lax
from jax.sharding import PartitionSpec as P

D = 2048
DK = 128
DV = 256
BLOCK = 64
AHEAD = 2
DOWN_CHUNKS = 2


epsilon = 1e-06
highest = lax.Precision.HIGHEST


def rms_rows(values, gain):
    values = values.astype(jnp.float32)
    factor = lax.rsqrt(jnp.mean(values * values, axis=-1, keepdims=True) + epsilon)
    return values * factor * gain


def blockwise_gla(query_rows, key_rows, value_rows, log_decay, head_count):
    length = query_rows.shape[0]
    blocks = length // BLOCK

    def split_heads(array, depth):
        return (
            array.astype(jnp.float32)
            .reshape(blocks, BLOCK, head_count, depth)
            .transpose(2, 0, 1, 3)
        )

    query_f = split_heads(query_rows, DK) * DK ** (-0.5)
    key_f = split_heads(key_rows, DK)
    value_f = split_heads(value_rows, DV)
    log_cum = jnp.cumsum(split_heads(log_decay, DK), axis=2)
    log_last = log_cum[:, :, -1:, :]
    query_dec = query_f * jnp.exp(log_cum)
    key_dec = key_f * jnp.exp(-log_cum)
    causal = jnp.tril(jnp.ones((BLOCK, BLOCK), dtype=bool))
    scores = jnp.where(
        causal, jnp.einsum("hncd,hnsd->hncs", query_dec, key_dec, precision=highest), 0.0
    )
    inside = jnp.einsum("hncs,hnsv->hncv", scores, value_f, precision=highest)
    contrib = jnp.einsum(
        "hncd,hncv->hndv", key_f * jnp.exp(log_last - log_cum), value_f, precision=highest
    )
    decay_block = jnp.exp(log_last[:, :, 0, :])

    def advance(carry_state, inputs):
        decay_step, added = inputs
        return (decay_step[..., None] * carry_state + added, carry_state)

    start_state = jnp.zeros((head_count, DK, DV), jnp.float32)
    final_state, earlier = lax.scan(
        advance, start_state, (jnp.moveaxis(decay_block, 1, 0), jnp.moveaxis(contrib, 1, 0))
    )
    earlier = jnp.moveaxis(earlier, 0, 1)
    output = inside + jnp.einsum("hncd,hndv->hncv", query_dec, earlier, precision=highest)
    return output.transpose(1, 2, 0, 3).reshape(length, head_count, DV)


def arrivals(place, count):
    order = []
    for step in range(1, count):
        if place >= step:
            order.append(("right", step))
        if place + step < count:
            order.append(("left", step))
    return order


def gather_pieces(piece, axes_size):
    count, groups = axes_size
    me = lax.axis_index("fs")
    moved = {("right", 0): piece, ("left", 0): piece}
    for step in range(1, count):
        moved["right", step] = lax.ppermute(
            moved["right", step - 1], "fs", [(i, i + 1) for i in range(step - 1, count - 1)]
        )
        moved["left", step] = lax.ppermute(
            moved["left", step - 1], "fs", [(i + 1, i) for i in range(count - step)]
        )
    slots = []
    for slot in range(count - 1):
        chosen = [arrivals(place, count)[slot] for place in range(count)]
        merged = moved[chosen[0]]
        for key in sorted(set(chosen) - {chosen[0]}):
            takers = [place for place in range(count) if chosen[place] == key]
            wanted = functools.reduce(jnp.logical_or, [me == place for place in takers])
            merged = jnp.where(wanted, moved[key], merged)
        merged = lax.optimization_barrier(merged)
        parts = [merged]
        for turn in range(1, groups):
            pairs = [(g, (g + turn) % groups) for g in range(groups)]
            parts.append(lax.ppermute(merged, "grp", pairs))
        slots.append(parts)
    return slots, (moved["right", count - 2], moved["left", count - 2])


def owner_of(slot, count):
    me = lax.axis_index("fs")
    owner = jnp.int32(0)
    for place in range(count):
        way, step = arrivals(place, count)[slot]
        owner = jnp.where(me == place, place - step if way == "right" else place + step, owner)
    return owner


def assemble(own, slots, axes_size, axis, size, spread, shift):
    count, groups = axes_size
    me, group = lax.axis_index("fs"), lax.axis_index("grp")
    whole = own
    for slot in range(count - 1):
        owner = owner_of(slot, count)
        for turn in range(groups):
            at = owner * size + lax.rem(group - turn + groups, groups) * spread + shift
            whole = lax.dynamic_update_slice_in_dim(whole, slots[slot][turn], at, axis)
    return whole


def room(weight, axes_size, axis):
    shape = list(weight.shape)
    shape[axis] *= axes_size[0]
    whole = jnp.zeros(tuple(shape), weight.dtype)
    return lax.dynamic_update_slice_in_dim(
        whole, weight, lax.axis_index("fs") * weight.shape[axis], axis
    )


def own_part(weight, groups, axis, chunk, chunks):
    spread = weight.shape[axis] // groups
    width = spread // chunks
    start = lax.axis_index("grp") * spread + chunk * width
    return lax.dynamic_slice_in_dim(weight, start, width, axis)


def body(
    axes_size,
    tokens,
    attn_gain,
    w_query,
    w_key,
    w_value,
    w_low,
    w_lift,
    decay_bias,
    head_gain,
    w_out,
    ffn_gain,
    w_gate,
    w_up,
    w_down,
    final_gain,
):
    own_width = tokens.shape[1]
    row_count = tokens.shape[0]
    groups = axes_size[1]
    w_mix = jnp.concatenate([w_query, w_key, w_value], axis=1)
    started = []

    def gather(weight, axis, chunks, after):
        size = weight.shape[axis]
        spread = size // groups
        if spread % (128 * chunks):
            chunks = 1
        whole = room(weight, axes_size, axis)
        for chunk in range(chunks):
            part = own_part(weight, groups, axis, chunk, chunks)
            held = list(after[min(chunk, len(after) - 1)]) if after else []
            if len(started) >= AHEAD:
                held += list(started[-AHEAD])
            if held:
                part = lax.optimization_barrier((part, *held))[0]
            slots, _ = gather_pieces(part, axes_size)
            started.append(slots[-1])
            whole = assemble(whole, slots, axes_size, axis, size, spread, chunk * (spread // chunks))
        return whole

    def product(source, weight):
        return jnp.dot(source, weight, preferred_element_type=jnp.float32)

    full_mix = gather(w_mix, 0, 1, ())
    full_out = gather(w_out, 1, 1, ())
    whole_rows = lax.all_gather(tokens, "tp", axis=1, tiled=True)
    normed = rms_rows(whole_rows, attn_gain).astype(jnp.bfloat16)
    full_gate = gather(w_gate, 0, 1, ((normed,),))
    mix = product(normed, full_mix).astype(jnp.bfloat16)
    keys_width = w_query.shape[1]
    query_rows, key_rows, value_rows = jnp.split(mix, [keys_width, 2 * keys_width], axis=1)
    low_rank = product(normed, w_low).astype(jnp.bfloat16)
    log_decay = jax.nn.log_sigmoid(product(low_rank, w_lift) + decay_bias) / 16.0
    full_up = gather(w_up, 0, 1, ((mix, log_decay),))
    head_count = query_rows.shape[1] // DK
    gla_out = blockwise_gla(query_rows, key_rows, value_rows, log_decay, head_count)
    mixed_heads = (
        rms_rows(gla_out, head_gain).reshape(row_count, head_count * DV).astype(jnp.bfloat16)
    )
    out_terms = product(mixed_heads, full_out).astype(jnp.bfloat16)
    total_sum = lax.psum(out_terms, "tp").astype(jnp.float32)
    full_rows = (whole_rows.astype(jnp.float32) + total_sum).astype(jnp.bfloat16)
    first_sum = lax.dynamic_slice_in_dim(full_rows, lax.axis_index("tp") * own_width, own_width, 1)
    normed_ffn = rms_rows(full_rows, ffn_gain).astype(jnp.bfloat16)
    full_down = gather(w_down, 1, DOWN_CHUNKS, ((out_terms,), (normed_ffn,)))
    gate_rows = product(normed_ffn, full_gate)
    up_rows = product(normed_ffn, full_up)
    hidden = (jax.nn.silu(gate_rows) * up_rows).astype(jnp.bfloat16)
    down_terms = product(hidden, full_down)
    own_ffn = lax.psum_scatter(
        down_terms.astype(jnp.bfloat16), "tp", scatter_dimension=1, tiled=True
    ).astype(jnp.float32)
    second_sum = first_sum.astype(jnp.float32) + own_ffn
    square_sum = lax.psum(jnp.sum(second_sum * second_sum, axis=1), "tp")
    factor = lax.rsqrt(square_sum / D + epsilon)[:, None]
    return (second_sum * factor * final_gain).astype(jnp.bfloat16)


def solution(mesh):
    axes_size = (mesh.shape["fs"], mesh.shape["grp"])
    return jax.shard_map(
        functools.partial(body, axes_size),
        mesh=mesh,
        in_specs=(
            P(("grp", "fs"), "tp"),
            P(),
            P("fs", "tp"),
            P("fs", "tp"),
            P("fs", "tp"),
            P(),
            P(None, "tp"),
            P("tp"),
            P(),
            P("tp", "fs"),
            P(),
            P("fs", "tp"),
            P("fs", "tp"),
            P("tp", "fs"),
            P("tp"),
        ),
        out_specs=P(("grp", "fs"), "tp"),
        check_vma=False,
    )
```

```python
import functools

import jax
import jax.numpy as jnp
from jax import lax
from jax.experimental import pallas as pl
from jax.experimental.pallas import tpu as pltpu
from jax.sharding import PartitionSpec as P

DK = 128
DV = 256
BLOCK = 64
epsilon = 1e-06
highest = lax.Precision.HIGHEST
MESH = pl.DeviceIdType.MESH
DOWN_CHUNKS = 2


def layer_kernel(
    sizes,
    tokens_ref,
    attn_gain_ref,
    w_low_ref,
    w_lift_ref,
    decay_bias_ref,
    head_gain_ref,
    ffn_gain_ref,
    final_gain_ref,
    w_mix_ref,
    w_out_ref,
    w_gate_ref,
    w_up_ref,
    w_down_ref,
    result_ref,
    g_mix,
    g_out,
    g_gate,
    g_up,
    g_down,
    rows_all,
    normed,
    mix_rows,
    log_decay,
    mixed,
    state,
    partial_out,
    heard_out,
    first_all,
    gate_acc,
    up_acc,
    hidden,
    partial_down,
    heard_down,
    squares,
    z_send,
    z_recv,
    y_send,
    y_recv,
    tp_send,
    tp_recv,
    local_sem,
):
    n, tp = sizes
    g, f, t = lax.axis_index("grp"), lax.axis_index("fs"), lax.axis_index("tp")
    rows, width = tokens_ref.shape
    features = width * tp
    f32 = jnp.float32

    weights = [(w_mix_ref, g_mix), (w_out_ref, g_out), (w_gate_ref, g_gate), (w_up_ref, g_up)]
    messages = [(w, held, 0, 1) for w, held in weights]
    messages += [(w_down_ref, g_down, c, DOWN_CHUNKS) for c in range(DOWN_CHUNKS)]

    barrier = pltpu.get_barrier_semaphore()

    @pl.when(f > 0)
    def _():
        pl.semaphore_signal(barrier, inc=1, device_id=(g, f - 1, t), device_id_type=MESH)

    @pl.when(f < n - 1)
    def _():
        pl.semaphore_signal(barrier, inc=1, device_id=(g, f + 1, t), device_id_type=MESH)

    pl.semaphore_signal(barrier, inc=1, device_id=(1 - g, f, t), device_id_type=MESH)
    for d in range(1, tp):
        peer = lax.rem(t + d, tp)
        pl.semaphore_signal(barrier, inc=1, device_id=(g, f, peer), device_id_type=MESH)
    met = jnp.where(f > 0, 1, 0) + jnp.where(f < n - 1, 1, 0) + tp
    pl.semaphore_wait(barrier, met)

    def span(m, group):
        w, _, chunk, chunks = messages[m]
        part = w.shape[0] // 2
        length = part // chunks
        return pl.ds(pl.multiple_of(group * part + chunk * length, 16), length)

    def z_copy(m, way, step):
        w, held, _, _ = messages[m]
        owner = f - (step - 1) if way == 0 else f + (step - 1)
        at = held.at[owner, span(m, g)]
        source = w.at[span(m, g)] if step == 1 else at
        target = f + 1 if way == 0 else f - 1
        return pltpu.make_async_remote_copy(
            source, at, z_send.at[m, way, step], z_recv.at[m, way, step],
            device_id=(g, target, t), device_id_type=MESH,
        )

    def y_copy(m, way, step):
        held = messages[m][1]
        owner = f - step if way == 0 else f + step
        at = held.at[owner, span(m, g)]
        return pltpu.make_async_remote_copy(
            at, at, y_send.at[m, way, step], y_recv.at[m, way, step],
            device_id=(1 - g, f, t), device_id_type=MESH,
        )

    def gets(way, step):
        return f >= step if way == 0 else f + step < n

    def gives(way, step):
        if way == 0:
            return jnp.logical_and(f + 1 < n, f >= step - 1)
        return jnp.logical_and(f >= 1, f + step - 1 < n)

    def launch(m):
        for way in (0, 1):
            @pl.when(gives(way, 1))
            def _():
                z_copy(m, way, 1).start()

    def tick(m, step):
        for way in (0, 1):
            @pl.when(gets(way, step))
            def _():
                z_copy(m, way, step).wait_recv()
                y_copy(m, way, step).start()

            if step < n - 1:
                @pl.when(gives(way, step + 1))
                def _():
                    z_copy(m, way, step + 1).start()

    def arrived(m, way, step):
        y_copy(m, way, step).wait_recv()

    def all_arrived(m):
        for step in range(1, n):
            for way in (0, 1):
                @pl.when(gets(way, step))
                def _():
                    arrived(m, way, step)

    def tp_copy(kind, source, target, d, peer):
        return pltpu.make_async_remote_copy(
            source, target, tp_send.at[kind, d], tp_recv.at[kind, d],
            device_id=(g, f, peer), device_id_type=MESH,
        )

    def token_copy(d):
        return tp_copy(0, tokens_ref, rows_all.at[t], d, lax.rem(t + d, tp))

    def out_copy(d):
        peer = lax.rem(t + d, tp)
        return tp_copy(1, partial_out.at[peer], heard_out.at[d - 1], d, peer)

    def first_copy(d):
        return tp_copy(2, first_all.at[t], first_all.at[t], d, lax.rem(t + d, tp))

    def down_copy(d):
        peer = lax.rem(t + d, tp)
        return tp_copy(3, partial_down.at[peer], heard_down.at[d - 1], d, peer)

    def square_copy(d):
        return tp_copy(4, squares.at[0], squares.at[d], d, lax.rem(t + d, tp))

    others = range(1, tp)
    for d in others:
        token_copy(d).start()
    launch(0)
    launch(1)
    locals_ = [pltpu.make_async_copy(tokens_ref, rows_all.at[t], local_sem.at[0])]
    for index, (w, held) in enumerate(weights + [(w_down_ref, g_down)]):
        locals_.append(pltpu.make_async_copy(w, held.at[f], local_sem.at[index + 1]))
    for copy in locals_:
        copy.start()
    for copy in locals_:
        copy.wait()
    for d in others:
        token_copy(d).wait_recv()

    def normalize(source, gain_ref):
        total = jnp.zeros((rows, 1), f32)
        for p in range(tp):
            values = source[p].astype(f32)
            total += jnp.sum(values * values, axis=1, keepdims=True)
        factor = lax.rsqrt(total / features + epsilon)
        for p in range(tp):
            part = pl.ds(p * width, width)
            scaled = source[p].astype(f32) * factor * gain_ref[:, part]
            normed[:, part] = scaled.astype(jnp.bfloat16)

    def accumulate(held, acc):
        depth = held.shape[1]
        acc[...] = jnp.zeros_like(acc)

        def step(j, carry):
            columns = pl.ds(pl.multiple_of(j * depth, 128), depth)
            acc[...] += jnp.dot(normed[:, columns], held[j], preferred_element_type=f32)
            return carry

        lax.fori_loop(0, n, step, 0)

    normalize(rows_all, attn_gain_ref)
    low_rank = jnp.dot(normed[...], w_low_ref[...], preferred_element_type=f32)
    lifted = jnp.dot(low_rank.astype(jnp.bfloat16), w_lift_ref[...], preferred_element_type=f32)
    log_decay[...] = jax.nn.log_sigmoid(lifted + decay_bias_ref[...]) / 16.0

    def pair(a, b, after):
        for step in range(1, n):
            tick(a, step)
            tick(b, step)
            if step == max(n - 2, 1):
                for m in after:
                    launch(m)

    pair(0, 1, (2, 3))
    all_arrived(0)
    mix_acc = up_acc.at[:, pl.ds(0, mix_rows.shape[1])]
    accumulate(g_mix, mix_acc)
    mix_rows[...] = mix_acc[...].astype(jnp.bfloat16)

    heads = mix_rows.shape[1] // (2 * DK + DV)
    at_row = lax.broadcasted_iota(jnp.int32, (BLOCK, BLOCK), 0)
    at_col = lax.broadcasted_iota(jnp.int32, (BLOCK, BLOCK), 1)
    causal = at_row >= at_col
    lower = causal.astype(f32)

    def dot(a, b, ca, cb):
        return lax.dot_general(
            a, b, (((ca,), (cb,)), ((), ())), precision=highest, preferred_element_type=f32
        )

    state[...] = jnp.zeros_like(state)

    def block_step(block, carry):
        here = pl.ds(pl.multiple_of(block * BLOCK, BLOCK), BLOCK)
        for h in range(heads):
            query = mix_rows[here, pl.ds(h * DK, DK)].astype(f32) * DK ** (-0.5)
            key = mix_rows[here, pl.ds((heads + h) * DK, DK)].astype(f32)
            value = mix_rows[here, pl.ds(2 * heads * DK + h * DV, DV)].astype(f32)
            cum = dot(lower, log_decay[here, pl.ds(h * DK, DK)], 1, 0)
            last = cum[BLOCK - 1 :, :]
            query_dec = query * jnp.exp(cum)
            key_dec = key * jnp.exp(-cum)
            scores = jnp.where(causal, dot(query_dec, key_dec, 1, 1), 0.0)
            held = state[h]
            out = dot(scores, value, 1, 0) + dot(query_dec, held, 1, 0)
            decay = jnp.transpose(jnp.broadcast_to(jnp.exp(last), (DK, DK)))
            decay = jnp.concatenate([decay] * (DV // DK), axis=1)
            state[h] = decay * held + dot(key * jnp.exp(last - cum), value, 0, 0)
            factor = lax.rsqrt(jnp.mean(out * out, axis=1, keepdims=True) + epsilon)
            mixed[here, pl.ds(h * DV, DV)] = (out * factor * head_gain_ref[...]).astype(jnp.bfloat16)
        return carry

    lax.fori_loop(0, rows // BLOCK, block_step, 0)
    if n > 2:
        tick(2, 1)
    all_arrived(1)

    def block_place(j, columns):
        return j * columns // width, pl.ds(pl.multiple_of(lax.rem(j * columns, width), 128), columns)

    def out_step(j, carry):
        p, part = block_place(j, g_out.shape[2])
        terms = jnp.dot(mixed[...], g_out[j], preferred_element_type=f32)
        partial_out[p, :, part] = terms.astype(jnp.bfloat16)
        return carry

    lax.fori_loop(0, n, out_step, 0)
    for d in others:
        out_copy(d).start()
    if n > 2:
        tick(3, 1)
    for d in others:
        out_copy(d).wait_recv()
    total = partial_out[t].astype(f32)
    for d in others:
        total += heard_out[d - 1].astype(f32)
    first_all[t] = (rows_all[t].astype(f32) + total).astype(jnp.bfloat16)
    for d in others:
        first_copy(d).start()
    for step in range(2, n - 1):
        tick(2, step)
        tick(3, step)
    launch(4)
    launch(5)
    for d in others:
        first_copy(d).wait_recv()
    normalize(first_all, ffn_gain_ref)
    tick(2, n - 1)
    all_arrived(2)
    accumulate(g_gate, gate_acc)
    tick(3, n - 1)
    tick(4, 1)
    all_arrived(3)
    accumulate(g_up, up_acc)
    gate = gate_acc[...]
    hidden[...] = (gate / (1.0 + jnp.exp(-gate)) * up_acc[...]).astype(jnp.bfloat16)
    eager = g_down.shape[2] == width

    def down_block(j):
        p, part = block_place(j, g_down.shape[2])
        terms = jnp.dot(hidden[...], g_down[j], preferred_element_type=f32)
        partial_down[p, :, part] = terms.astype(jnp.bfloat16)
        if eager:
            for d in others:
                @pl.when(j == lax.rem(t + d, tp))
                def _():
                    down_copy(d).start()

    down_block(f)
    for step in range(1, n):
        if step > 1:
            tick(4, step)
        tick(5, step)
        for way in (0, 1):
            @pl.when(gets(way, step))
            def _():
                arrived(4, way, step)
                arrived(5, way, step)
                down_block(f - step if way == 0 else f + step)
    if not eager:
        for d in others:
            down_copy(d).start()
    for d in others:
        down_copy(d).wait_recv()
    second = partial_down[t].astype(f32)
    for d in others:
        second += heard_down[d - 1].astype(f32)
    second = first_all[t].astype(f32) + second
    ones = jnp.ones((8, width), f32)
    squares[0] = dot(ones, second * second, 1, 1)
    for d in others:
        square_copy(d).start()
    for d in others:
        square_copy(d).wait_recv()
    whole = squares[0]
    for d in others:
        whole += squares[d]
    factor = lax.rsqrt(jnp.transpose(whole) / features + epsilon)[:, :1]
    result_ref[...] = (second * factor * final_gain_ref[...]).astype(jnp.bfloat16)

    for m in range(len(messages)):
        for step in range(1, n):
            for way in (0, 1):
                @pl.when(gives(way, step))
                def _():
                    z_copy(m, way, step).wait_send()

                @pl.when(gets(way, step))
                def _():
                    y_copy(m, way, step).wait_send()
    for d in others:
        for copy in (token_copy, out_copy, first_copy, down_copy, square_copy):
            copy(d).wait_send()


def body(
    sizes, tokens, attn_gain, w_query, w_key, w_value, w_low, w_lift, decay_bias, head_gain,
    w_out, ffn_gain, w_gate, w_up, w_down, final_gain,
):
    n, tp = sizes
    rows, width = tokens.shape
    w_mix = jnp.concatenate([w_query, w_key, w_value], axis=1)
    bf16, f32 = jnp.bfloat16, jnp.float32
    units, mix_width, keys = w_gate.shape[1], w_mix.shape[1], w_query.shape[1]
    values = w_value.shape[1]
    held = [pltpu.VMEM((n, *w.shape), bf16) for w in (w_mix, w_out, w_gate, w_up, w_down)]
    messages = 4 + DOWN_CHUNKS
    dma = pltpu.SemaphoreType.DMA
    anywhere = pl.BlockSpec(memory_space=pl.ANY)
    inside = pl.BlockSpec(memory_space=pltpu.VMEM)
    return pl.pallas_call(
        functools.partial(layer_kernel, sizes),
        name="layer",
        out_shape=jax.ShapeDtypeStruct((rows, width), bf16),
        in_specs=[anywhere] + [inside] * 7 + [anywhere] * 5,
        out_specs=inside,
        scratch_shapes=held + [
            pltpu.VMEM((tp, rows, width), bf16),
            pltpu.VMEM((rows, width * tp), bf16),
            pltpu.VMEM((rows, mix_width), bf16),
            pltpu.VMEM((rows, keys), f32),
            pltpu.VMEM((rows, values), bf16),
            pltpu.VMEM((keys // DK, DK, DV), f32),
            pltpu.VMEM((tp, rows, width), bf16),
            pltpu.VMEM((tp - 1, rows, width), bf16),
            pltpu.VMEM((tp, rows, width), bf16),
            pltpu.VMEM((rows, units), f32),
            pltpu.VMEM((rows, units), f32),
            pltpu.VMEM((rows, units), bf16),
            pltpu.VMEM((tp, rows, width), bf16),
            pltpu.VMEM((tp - 1, rows, width), bf16),
            pltpu.VMEM((tp, 8, rows), f32),
            dma((messages, 2, n)),
            dma((messages, 2, n)),
            dma((messages, 2, n)),
            dma((messages, 2, n)),
            dma((5, tp)),
            dma((5, tp)),
            dma((6,)),
        ],
        compiler_params=pltpu.CompilerParams(
            collective_id=0, has_side_effects=True, vmem_limit_bytes=63 * 1024 * 1024
        ),
    )(
        tokens, attn_gain[None], w_low, w_lift, decay_bias[None], head_gain[None],
        ffn_gain[None], final_gain[None], w_mix, w_out, w_gate, w_up, w_down,
    )


def solution(mesh):
    sizes = (mesh.shape["fs"], mesh.shape["tp"])
    return jax.shard_map(
        functools.partial(body, sizes),
        mesh=mesh,
        in_specs=(
            P(("grp", "fs"), "tp"),
            P(),
            P("fs", "tp"),
            P("fs", "tp"),
            P("fs", "tp"),
            P(),
            P(None, "tp"),
            P("tp"),
            P(),
            P("tp", "fs"),
            P(),
            P("fs", "tp"),
            P("fs", "tp"),
            P("tp", "fs"),
            P("tp"),
        ),
        out_specs=P(("grp", "fs"), "tp"),
        check_vma=False,
    )
```

```python
import functools

import jax
import jax.numpy as jnp
from jax import lax
from jax.experimental import pallas as pl
from jax.experimental.pallas import tpu as pltpu
from jax.sharding import PartitionSpec as P

DK = 128
DV = 256
BLOCK = 64
epsilon = 1e-06
highest = lax.Precision.HIGHEST
MESH = pl.DeviceIdType.MESH
LANES = 128


def layer_kernel(
    sizes,
    tokens_ref,
    attn_gain_ref,
    w_low_ref,
    w_lift_ref,
    decay_bias_ref,
    head_gain_ref,
    ffn_gain_ref,
    final_gain_ref,
    w_query_ref,
    w_key_ref,
    w_value_ref,
    w_out_ref,
    w_gate_ref,
    w_up_ref,
    w_down_ref,
    result_ref,
    g_mix,
    g_out,
    g_gate,
    g_up,
    g_down,
    rows_all,
    normed,
    mix_rows,
    log_decay,
    mixed,
    state,
    partial_out,
    heard_out,
    first_all,
    gate_acc,
    up_acc,
    hidden,
    partial_down,
    heard_down,
    squares,
    down_send,
    down_recv,
    z_send,
    z_recv,
    y_send,
    y_recv,
    tp_send,
    tp_recv,
    local_sem,
):
    n, tp = sizes
    g, f, t = lax.axis_index("grp"), lax.axis_index("fs"), lax.axis_index("tp")
    rows, width = tokens_ref.shape
    features = width * tp
    f32 = jnp.float32

    messages, owned = [], []
    for group in (
        ((w_query_ref, w_key_ref, w_value_ref), g_mix),
        ((w_out_ref,), g_out),
        ((w_gate_ref,), g_gate),
        ((w_up_ref,), g_up),
    ):
        column = 0
        for w in group[0]:
            messages.append((w, group[1], 0, column, w.shape[1]))
            owned.append(messages[-1])
            column += w.shape[1]
    chunks = w_down_ref.shape[1] // LANES
    owned.append((w_down_ref, g_down, 0, 0, w_down_ref.shape[1]))
    first_down = len(messages)
    messages += [(w_down_ref, g_down, c * LANES, c * LANES, LANES) for c in range(chunks)]
    opening, middle = range(4), range(4, first_down)
    closing = range(first_down, len(messages))

    barrier = pltpu.get_barrier_semaphore()

    @pl.when(f > 0)
    def _():
        pl.semaphore_signal(barrier, inc=1, device_id=(g, f - 1, t), device_id_type=MESH)

    @pl.when(f < n - 1)
    def _():
        pl.semaphore_signal(barrier, inc=1, device_id=(g, f + 1, t), device_id_type=MESH)

    pl.semaphore_signal(barrier, inc=1, device_id=(1 - g, f, t), device_id_type=MESH)
    for d in range(1, tp):
        peer = lax.rem(t + d, tp)
        pl.semaphore_signal(barrier, inc=1, device_id=(g, f, peer), device_id_type=MESH)
    met = jnp.where(f > 0, 1, 0) + jnp.where(f < n - 1, 1, 0) + tp
    pl.semaphore_wait(barrier, met)

    def z_copy(m, way, step):
        w, held, start, column, columns = messages[m]
        owner = f - (step - 1) if way == 0 else f + (step - 1)
        part = w.shape[0] // 2
        half = pl.ds(pl.multiple_of(g * part, 16), part)
        at = held.at[owner, half, pl.ds(column, columns)]
        source = w.at[half, pl.ds(start, columns)] if step == 1 else at
        target = f + 1 if way == 0 else f - 1
        return pltpu.make_async_remote_copy(
            source, at, z_send.at[m, way, step], z_recv.at[m, way, step],
            device_id=(g, target, t), device_id_type=MESH,
        )

    def y_copy(m, way, step):
        w, held, _, column, columns = messages[m]
        part = w.shape[0] // 2
        half = pl.ds(pl.multiple_of(g * part, 16), part)
        at = held.at[f + step * (2 * way - 1), half, pl.ds(column, columns)]
        return pltpu.make_async_remote_copy(
            at, at, y_send.at[m, way, step], y_recv.at[m, way, step],
            device_id=(1 - g, f, t), device_id_type=MESH,
        )

    def gets(way, step):
        return f >= step if way == 0 else f + step < n

    def gives(way, step):
        if way == 0:
            return jnp.logical_and(f + 1 < n, f >= step - 1)
        return jnp.logical_and(f >= 1, f + step - 1 < n)

    def launch(m):
        for way in (0, 1):
            @pl.when(gives(way, 1))
            def _():
                z_copy(m, way, 1).start()

    def tick(m, step):
        for way in (0, 1):
            @pl.when(gets(way, step))
            def _():
                z_copy(m, way, step).wait_recv()
                y_copy(m, way, step).start()

            if step < n - 1:
                @pl.when(gives(way, step + 1))
                def _():
                    z_copy(m, way, step + 1).start()

    def arrived(m, way, step):
        y_copy(m, way, step).wait_recv()

    def all_arrived(m):
        for step in range(1, n):
            for way in (0, 1):
                @pl.when(gets(way, step))
                def _():
                    arrived(m, way, step)

    def tp_copy(kind, source, target, d, peer):
        return pltpu.make_async_remote_copy(
            source, target, tp_send.at[kind, d], tp_recv.at[kind, d],
            device_id=(g, f, peer), device_id_type=MESH,
        )

    def token_copy(d):
        return tp_copy(0, tokens_ref, rows_all.at[t], d, lax.rem(t + d, tp))

    def out_copy(d):
        peer = lax.rem(t + d, tp)
        return tp_copy(1, partial_out.at[peer], heard_out.at[d - 1], d, peer)

    def first_copy(d):
        return tp_copy(2, first_all.at[t], first_all.at[t], d, lax.rem(t + d, tp))

    def down_copy(d, c):
        peer = lax.rem(t + d, tp)
        part = pl.ds(c * (width // chunks), width // chunks)
        return pltpu.make_async_remote_copy(
            partial_down.at[peer, :, part], heard_down.at[d - 1, :, part],
            down_send.at[c, d], down_recv.at[c, d],
            device_id=(g, f, peer), device_id_type=MESH,
        )

    def square_copy(d):
        return tp_copy(3, squares.at[0], squares.at[d], d, lax.rem(t + d, tp))

    others = range(1, tp)
    for m in opening:
        launch(m)
    for d in others:
        token_copy(d).start()
    locals_ = [pltpu.make_async_copy(tokens_ref, rows_all.at[t], local_sem.at[0])]
    for index, (w, held, _, column, columns) in enumerate(owned):
        at = held.at[f, :, pl.ds(column, columns)]
        locals_.append(pltpu.make_async_copy(w, at, local_sem.at[index + 1]))
    for copy in locals_:
        copy.start()

    for step in range(1, max(n - 1, 2)):
        for m in opening:
            tick(m, step)
    for m in middle:
        launch(m)
    for copy in locals_:
        copy.wait()
    for d in others:
        token_copy(d).wait_recv()

    def normalize(source, gain_ref):
        total = jnp.zeros((rows, 1), f32)
        for p in range(tp):
            values = source[p].astype(f32)
            total += jnp.sum(values * values, axis=1, keepdims=True)
        factor = lax.rsqrt(total / features + epsilon)
        for p in range(tp):
            part = pl.ds(p * width, width)
            scaled = source[p].astype(f32) * factor * gain_ref[:, part]
            normed[:, part] = scaled.astype(jnp.bfloat16)

    def accumulate(held, acc):
        depth = held.shape[1]
        acc[...] = jnp.zeros_like(acc)

        def step(j, carry):
            columns = pl.ds(pl.multiple_of(j * depth, 128), depth)
            acc[...] += jnp.dot(normed[:, columns], held[j], preferred_element_type=f32)
            return carry

        lax.fori_loop(0, n, step, 0)

    normalize(rows_all, attn_gain_ref)
    low_rank = lax.dot_general(
        normed[...], w_low_ref[...], (((1,), (1,)), ((), ())), preferred_element_type=f32
    )
    lifted = jnp.dot(low_rank.astype(jnp.bfloat16), w_lift_ref[...], preferred_element_type=f32)
    log_decay[...] = jax.nn.log_sigmoid(lifted + decay_bias_ref[...]) / 16.0

    if n > 2:
        for m in opening:
            tick(m, n - 1)
    for m in range(3):
        all_arrived(m)
    mix_acc = up_acc.at[:, pl.ds(0, mix_rows.shape[1])]
    accumulate(g_mix, mix_acc)
    mix_rows[...] = mix_acc[...].astype(jnp.bfloat16)

    heads = mix_rows.shape[1] // (2 * DK + DV)
    at_row = lax.broadcasted_iota(jnp.int32, (BLOCK, BLOCK), 0)
    at_col = lax.broadcasted_iota(jnp.int32, (BLOCK, BLOCK), 1)
    causal = at_row >= at_col
    lower = causal.astype(f32)

    def dot(a, b, ca, cb):
        return lax.dot_general(
            a, b, (((ca,), (cb,)), ((), ())), precision=highest, preferred_element_type=f32
        )

    state[...] = jnp.zeros_like(state)

    def block_step(block, carry):
        here = pl.ds(pl.multiple_of(block * BLOCK, BLOCK), BLOCK)
        for h in range(heads):
            query = mix_rows[here, pl.ds(h * DK, DK)].astype(f32) * DK ** (-0.5)
            key = mix_rows[here, pl.ds((heads + h) * DK, DK)].astype(f32)
            value = mix_rows[here, pl.ds(2 * heads * DK + h * DV, DV)].astype(f32)
            cum = dot(lower, log_decay[here, pl.ds(h * DK, DK)], 1, 0)
            last = cum[BLOCK - 1 :, :]
            query_dec = query * jnp.exp(cum)
            key_dec = key * jnp.exp(-cum)
            scores = jnp.where(causal, dot(query_dec, key_dec, 1, 1), 0.0)
            held = state[h]
            out = dot(scores, value, 1, 0) + dot(query_dec, held, 1, 0)
            decay = jnp.transpose(jnp.broadcast_to(jnp.exp(last), (DK, DK)))
            decay = jnp.concatenate([decay] * (DV // DK), axis=1)
            state[h] = decay * held + dot(key * jnp.exp(last - cum), value, 0, 0)
            factor = lax.rsqrt(jnp.mean(out * out, axis=1, keepdims=True) + epsilon)
            mixed[here, pl.ds(h * DV, DV)] = (out * factor * head_gain_ref[...]).astype(jnp.bfloat16)
        return carry

    lax.fori_loop(0, rows // BLOCK, block_step, 0)
    gate_at, up_at = middle
    if n > 2:
        tick(gate_at, 1)
    all_arrived(3)

    def block_place(j, columns):
        return j * columns // width, pl.ds(pl.multiple_of(lax.rem(j * columns, width), 128), columns)

    def out_step(j, carry):
        p, part = block_place(j, g_out.shape[2])
        terms = jnp.dot(mixed[...], g_out[j], preferred_element_type=f32)
        partial_out[p, :, part] = terms.astype(jnp.bfloat16)
        return carry

    lax.fori_loop(0, n, out_step, 0)
    for d in others:
        out_copy(d).start()
    if n > 2:
        tick(up_at, 1)
    for d in others:
        out_copy(d).wait_recv()
    total = partial_out[t].astype(f32)
    for d in others:
        total += heard_out[d - 1].astype(f32)
    first_all[t] = (rows_all[t].astype(f32) + total).astype(jnp.bfloat16)
    for d in others:
        first_copy(d).start()
    for step in range(2, n - 1):
        tick(gate_at, step)
        tick(up_at, step)
    for m in closing:
        launch(m)
    for d in others:
        first_copy(d).wait_recv()
    normalize(first_all, ffn_gain_ref)
    tick(gate_at, n - 1)
    all_arrived(gate_at)
    accumulate(g_gate, gate_acc)
    tick(up_at, n - 1)
    for m in closing:
        tick(m, 1)
    all_arrived(up_at)
    accumulate(g_up, up_acc)
    gate = gate_acc[...]
    hidden[...] = (gate / (1.0 + jnp.exp(-gate)) * up_acc[...]).astype(jnp.bfloat16)
    eager = g_down.shape[2] == width

    def down_block(j, c):
        place = j * g_down.shape[2] + c * LANES
        p, part = place // width, pl.ds(pl.multiple_of(lax.rem(place, width), LANES), LANES)
        columns = pl.ds(c * LANES, LANES)
        terms = jnp.dot(hidden[...], g_down[j, :, columns], preferred_element_type=f32)
        partial_down[p, :, part] = terms.astype(jnp.bfloat16)
        if eager:
            for d in others:
                @pl.when(j == lax.rem(t + d, tp))
                def _():
                    down_copy(d, c).start()

    for c in range(chunks):
        down_block(f, c)
    for step in range(1, n):
        if step > 1:
            for m in closing:
                tick(m, step)
        for c, m in enumerate(closing):
            def from_way(way, carry):
                j = f + step * (2 * way - 1)

                @pl.when(jnp.logical_and(j >= 0, j < n))
                def _():
                    y_copy(m, way, step).wait_recv()
                    down_block(j, c)

                return carry

            lax.fori_loop(0, 2, from_way, 0)
    if not eager:
        for d in others:
            for c in range(chunks):
                down_copy(d, c).start()
    for d in others:
        for c in range(chunks):
            down_copy(d, c).wait_recv()
    second = partial_down[t].astype(f32)
    for d in others:
        second += heard_down[d - 1].astype(f32)
    second = first_all[t].astype(f32) + second
    ones = jnp.ones((8, width), f32)
    squares[0] = dot(ones, second * second, 1, 1)
    for d in others:
        square_copy(d).start()
    for d in others:
        square_copy(d).wait_recv()
    whole = squares[0]
    for d in others:
        whole += squares[d]
    factor = lax.rsqrt(jnp.transpose(whole) / features + epsilon)[:, :1]
    result_ref[...] = (second * factor * final_gain_ref[...]).astype(jnp.bfloat16)

    for m in range(len(messages)):
        for step in range(1, n):
            for way in (0, 1):
                @pl.when(gives(way, step))
                def _():
                    z_copy(m, way, step).wait_send()

                @pl.when(gets(way, step))
                def _():
                    y_copy(m, way, step).wait_send()
    for d in others:
        for copy in (token_copy, out_copy, first_copy, square_copy):
            copy(d).wait_send()
        for c in range(chunks):
            down_copy(d, c).wait_send()


def body(
    sizes, tokens, attn_gain, w_query, w_key, w_value, w_low, w_lift, decay_bias, head_gain,
    w_out, ffn_gain, w_gate, w_up, w_down, final_gain,
):
    n, tp = sizes
    rows, width = tokens.shape
    bf16, f32 = jnp.bfloat16, jnp.float32
    units, keys, values = w_gate.shape[1], w_query.shape[1], w_value.shape[1]
    mix_width = 2 * keys + values
    held = [pltpu.VMEM((n, w_query.shape[0], mix_width), bf16)]
    held += [pltpu.VMEM((n, *w.shape), bf16) for w in (w_out, w_gate, w_up, w_down)]
    chunks = w_down.shape[1] // LANES
    messages = 6 + chunks
    dma = pltpu.SemaphoreType.DMA
    anywhere = pl.BlockSpec(memory_space=pl.ANY)
    inside = pl.BlockSpec(memory_space=pltpu.VMEM)
    return pl.pallas_call(
        functools.partial(layer_kernel, sizes),
        name="layer",
        out_shape=jax.ShapeDtypeStruct((rows, width), bf16),
        in_specs=[anywhere] + [inside] * 7 + [anywhere] * 7,
        out_specs=inside,
        scratch_shapes=held + [
            pltpu.VMEM((tp, rows, width), bf16),
            pltpu.VMEM((rows, width * tp), bf16),
            pltpu.VMEM((rows, mix_width), bf16),
            pltpu.VMEM((rows, keys), f32),
            pltpu.VMEM((rows, values), bf16),
            pltpu.VMEM((keys // DK, DK, DV), f32),
            pltpu.VMEM((tp, rows, width), bf16),
            pltpu.VMEM((tp - 1, rows, width), bf16),
            pltpu.VMEM((tp, rows, width), bf16),
            pltpu.VMEM((rows, units), f32),
            pltpu.VMEM((rows, units), f32),
            pltpu.VMEM((rows, units), bf16),
            pltpu.VMEM((tp, rows, width), bf16),
            pltpu.VMEM((tp - 1, rows, width), bf16),
            pltpu.VMEM((tp, 8, rows), f32),
            dma((chunks, tp)),
            dma((chunks, tp)),
            dma((messages, 2, n)),
            dma((messages, 2, n)),
            dma((messages, 2, n)),
            dma((messages, 2, n)),
            dma((4, tp)),
            dma((4, tp)),
            dma((8,)),
        ],
        compiler_params=pltpu.CompilerParams(
            collective_id=0, has_side_effects=True, vmem_limit_bytes=63 * 1024 * 1024
        ),
    )(
        tokens, attn_gain[None], w_low.T, w_lift, decay_bias[None], head_gain[None],
        ffn_gain[None], final_gain[None], w_query, w_key, w_value, w_out, w_gate, w_up, w_down,
    )


def solution(mesh):
    sizes = (mesh.shape["fs"], mesh.shape["tp"])
    return jax.shard_map(
        functools.partial(body, sizes),
        mesh=mesh,
        in_specs=(
            P(("grp", "fs"), "tp"),
            P(),
            P("fs", "tp"),
            P("fs", "tp"),
            P("fs", "tp"),
            P(),
            P(None, "tp"),
            P("tp"),
            P(),
            P("tp", "fs"),
            P(),
            P("fs", "tp"),
            P("fs", "tp"),
            P("tp", "fs"),
            P("tp"),
        ),
        out_specs=P(("grp", "fs"), "tp"),
        check_vma=False,
    )
```

```python
import functools

import jax
import jax.numpy as jnp
from jax import lax
from jax.experimental import pallas as pl
from jax.experimental.pallas import tpu as pltpu
from jax.sharding import PartitionSpec as P

DK = 128
DV = 256
BLOCK = 64
epsilon = 1e-06
highest = lax.Precision.HIGHEST
MESH = pl.DeviceIdType.MESH
LANES = 128


def layer_kernel(
    sizes,
    tokens_ref,
    attn_gain_ref,
    w_low_ref,
    w_lift_ref,
    decay_bias_ref,
    head_gain_ref,
    ffn_gain_ref,
    final_gain_ref,
    w_query_ref,
    w_key_ref,
    w_value_ref,
    w_out_ref,
    w_gate_ref,
    w_up_ref,
    w_down_ref,
    result_ref,
    g_mix,
    g_out,
    g_gate,
    g_up,
    g_down,
    rows_all,
    normed,
    mix_rows,
    log_decay,
    mixed,
    state,
    partial_out,
    heard_out,
    first_all,
    gate_acc,
    up_acc,
    hidden,
    partial_down,
    heard_down,
    squares,
    down_send,
    down_recv,
    z_send,
    z_recv,
    y_send,
    y_recv,
    tp_send,
    tp_recv,
    local_sem,
):
    n, tp = sizes
    g, f, t = lax.axis_index("grp"), lax.axis_index("fs"), lax.axis_index("tp")
    rows, width = tokens_ref.shape
    features = width * tp
    f32 = jnp.float32

    messages, owned = [], []
    for group in (
        ((w_query_ref, w_key_ref, w_value_ref), g_mix),
        ((w_out_ref,), g_out),
        ((w_gate_ref,), g_gate),
        ((w_up_ref,), g_up),
    ):
        column = 0
        for w in group[0]:
            messages.append((w, group[1], 0, column, w.shape[1]))
            owned.append(messages[-1])
            column += w.shape[1]
    chunks = w_down_ref.shape[1] // LANES
    owned.append((w_down_ref, g_down, 0, 0, w_down_ref.shape[1]))
    first_down = len(messages)
    messages += [(w_down_ref, g_down, c * LANES, c * LANES, LANES) for c in range(chunks)]
    opening, middle = range(4), range(4, first_down)
    closing = range(first_down, len(messages))

    barrier = pltpu.get_barrier_semaphore()

    @pl.when(f > 0)
    def _():
        pl.semaphore_signal(barrier, inc=1, device_id=(g, f - 1, t), device_id_type=MESH)

    @pl.when(f < n - 1)
    def _():
        pl.semaphore_signal(barrier, inc=1, device_id=(g, f + 1, t), device_id_type=MESH)

    pl.semaphore_signal(barrier, inc=1, device_id=(1 - g, f, t), device_id_type=MESH)
    for d in range(1, tp):
        peer = lax.rem(t + d, tp)
        pl.semaphore_signal(barrier, inc=1, device_id=(g, f, peer), device_id_type=MESH)
    met = jnp.where(f > 0, 1, 0) + jnp.where(f < n - 1, 1, 0) + tp
    pl.semaphore_wait(barrier, met)

    def z_copy(m, way, step):
        w, held, start, column, columns = messages[m]
        owner = f - (step - 1) if way == 0 else f + (step - 1)
        part = w.shape[0] // 2
        half = pl.ds(pl.multiple_of(g * part, 16), part)
        at = held.at[owner, half, pl.ds(column, columns)]
        source = w.at[half, pl.ds(start, columns)] if step == 1 else at
        target = f + 1 if way == 0 else f - 1
        return pltpu.make_async_remote_copy(
            source, at, z_send.at[m, way, step], z_recv.at[m, way, step],
            device_id=(g, target, t), device_id_type=MESH,
        )

    def y_copy(m, way, step):
        w, held, _, column, columns = messages[m]
        part = w.shape[0] // 2
        half = pl.ds(pl.multiple_of(g * part, 16), part)
        at = held.at[f + step * (2 * way - 1), half, pl.ds(column, columns)]
        return pltpu.make_async_remote_copy(
            at, at, y_send.at[m, way, step], y_recv.at[m, way, step],
            device_id=(1 - g, f, t), device_id_type=MESH,
        )

    def gets(way, step):
        return f >= step if way == 0 else f + step < n

    def gives(way, step):
        if way == 0:
            return jnp.logical_and(f + 1 < n, f >= step - 1)
        return jnp.logical_and(f >= 1, f + step - 1 < n)

    def launch(m):
        for way in (0, 1):
            @pl.when(gives(way, 1))
            def _():
                z_copy(m, way, 1).start()

    def tick(m, step):
        for way in (0, 1):
            @pl.when(gets(way, step))
            def _():
                z_copy(m, way, step).wait_recv()
                y_copy(m, way, step).start()

            if step < n - 1:
                @pl.when(gives(way, step + 1))
                def _():
                    z_copy(m, way, step + 1).start()

    def arrived(m, way, step):
        y_copy(m, way, step).wait_recv()

    def all_arrived(m):
        for step in range(1, n):
            for way in (0, 1):
                @pl.when(gets(way, step))
                def _():
                    arrived(m, way, step)

    def tp_copy(kind, source, target, d, peer):
        return pltpu.make_async_remote_copy(
            source, target, tp_send.at[kind, d], tp_recv.at[kind, d],
            device_id=(g, f, peer), device_id_type=MESH,
        )

    def token_copy(d):
        return tp_copy(0, tokens_ref, rows_all.at[t], d, lax.rem(t + d, tp))

    def out_copy(d):
        peer = lax.rem(t + d, tp)
        return tp_copy(1, partial_out.at[peer], heard_out.at[d - 1], d, peer)

    def first_copy(d):
        return tp_copy(2, first_all.at[t], first_all.at[t], d, lax.rem(t + d, tp))

    def down_copy(d, c):
        peer = lax.rem(t + d, tp)
        part = pl.ds(c * (width // chunks), width // chunks)
        return pltpu.make_async_remote_copy(
            partial_down.at[peer, :, part], heard_down.at[d - 1, :, part],
            down_send.at[c, d], down_recv.at[c, d],
            device_id=(g, f, peer), device_id_type=MESH,
        )

    def square_copy(d):
        return tp_copy(3, squares.at[0], squares.at[d], d, lax.rem(t + d, tp))

    others = range(1, tp)
    for m in opening:
        launch(m)
    for d in others:
        token_copy(d).start()
    locals_ = [pltpu.make_async_copy(tokens_ref, rows_all.at[t], local_sem.at[0])]
    for index, (w, held, _, column, columns) in enumerate(owned):
        at = held.at[f, :, pl.ds(column, columns)]
        locals_.append(pltpu.make_async_copy(w, at, local_sem.at[index + 1]))
    for copy in locals_:
        copy.start()

    for step in range(1, max(n - 1, 2)):
        for m in opening:
            tick(m, step)
    for m in middle:
        launch(m)
    for copy in locals_:
        copy.wait()
    for d in others:
        token_copy(d).wait_recv()

    def normalize(source, gain_ref):
        total = jnp.zeros((rows, 1), f32)
        for p in range(tp):
            values = source[p].astype(f32)
            total += jnp.sum(values * values, axis=1, keepdims=True)
        factor = lax.rsqrt(total / features + epsilon)
        for p in range(tp):
            part = pl.ds(p * width, width)
            scaled = source[p].astype(f32) * factor * gain_ref[:, part]
            normed[:, part] = scaled.astype(jnp.bfloat16)

    def accumulate(held, acc):
        depth = held.shape[1]
        acc[...] = jnp.zeros_like(acc)

        def step(j, carry):
            columns = pl.ds(pl.multiple_of(j * depth, 128), depth)
            acc[...] += jnp.dot(normed[:, columns], held[j], preferred_element_type=f32)
            return carry

        lax.fori_loop(0, n, step, 0)

    normalize(rows_all, attn_gain_ref)
    low_rank = lax.dot_general(
        normed[...], w_low_ref[...], (((1,), (1,)), ((), ())), preferred_element_type=f32
    )
    lifted = jnp.dot(low_rank.astype(jnp.bfloat16), w_lift_ref[...], preferred_element_type=f32)
    log_decay[...] = jax.nn.log_sigmoid(lifted + decay_bias_ref[...]) / 16.0

    if n > 2:
        for m in opening:
            tick(m, n - 1)
    for m in range(3):
        all_arrived(m)
    mix_acc = up_acc.at[:, pl.ds(0, mix_rows.shape[1])]
    accumulate(g_mix, mix_acc)
    mix_rows[...] = mix_acc[...].astype(jnp.bfloat16)

    heads = mix_rows.shape[1] // (2 * DK + DV)
    at_row = lax.broadcasted_iota(jnp.int32, (BLOCK, BLOCK), 0)
    at_col = lax.broadcasted_iota(jnp.int32, (BLOCK, BLOCK), 1)
    causal = at_row >= at_col
    lower = causal.astype(f32)

    def dot(a, b, ca, cb):
        return lax.dot_general(
            a, b, (((ca,), (cb,)), ((), ())), precision=highest, preferred_element_type=f32
        )

    state[...] = jnp.zeros_like(state)

    def block_step(block, carry):
        here = pl.ds(pl.multiple_of(block * BLOCK, BLOCK), BLOCK)
        for h in range(heads):
            query = mix_rows[here, pl.ds(h * DK, DK)].astype(f32) * DK ** (-0.5)
            key = mix_rows[here, pl.ds((heads + h) * DK, DK)].astype(f32)
            value = mix_rows[here, pl.ds(2 * heads * DK + h * DV, DV)].astype(f32)
            cum = dot(lower, log_decay[here, pl.ds(h * DK, DK)], 1, 0)
            last = cum[BLOCK - 1 :, :]
            query_dec = query * jnp.exp(cum)
            key_dec = key * jnp.exp(-cum)
            scores = jnp.where(causal, dot(query_dec, key_dec, 1, 1), 0.0)
            held = state[h]
            out = dot(scores, value, 1, 0) + dot(query_dec, held, 1, 0)
            decay = jnp.transpose(jnp.broadcast_to(jnp.exp(last), (DK, DK)))
            decay = jnp.concatenate([decay] * (DV // DK), axis=1)
            state[h] = decay * held + dot(key * jnp.exp(last - cum), value, 0, 0)
            factor = lax.rsqrt(jnp.mean(out * out, axis=1, keepdims=True) + epsilon)
            mixed[here, pl.ds(h * DV, DV)] = (out * factor * head_gain_ref[...]).astype(jnp.bfloat16)
        return carry

    gate_at, up_at = middle
    blocks = rows // BLOCK
    lax.fori_loop(0, blocks // 2, block_step, 0)
    if n > 2:
        tick(gate_at, 1)
    lax.fori_loop(blocks // 2, blocks, block_step, 0)
    all_arrived(3)

    def block_place(j, columns):
        return j * columns // width, pl.ds(pl.multiple_of(lax.rem(j * columns, width), 128), columns)

    def out_step(j, carry):
        p, part = block_place(j, g_out.shape[2])
        terms = jnp.dot(mixed[...], g_out[j], preferred_element_type=f32)
        partial_out[p, :, part] = terms.astype(jnp.bfloat16)
        return carry

    lax.fori_loop(0, n, out_step, 0)
    for d in others:
        out_copy(d).start()
    if n > 2:
        tick(up_at, 1)
    if n > 3:
        tick(gate_at, 2)
    for d in others:
        out_copy(d).wait_recv()
    total = partial_out[t].astype(f32)
    for d in others:
        total += heard_out[d - 1].astype(f32)
    first_all[t] = (rows_all[t].astype(f32) + total).astype(jnp.bfloat16)
    for d in others:
        first_copy(d).start()
    for step in range(2, n - 1):
        if step > 2:
            tick(gate_at, step)
        tick(up_at, step)
    for m in closing:
        launch(m)
    for d in others:
        first_copy(d).wait_recv()
    normalize(first_all, ffn_gain_ref)
    tick(gate_at, n - 1)
    all_arrived(gate_at)
    accumulate(g_gate, gate_acc)
    tick(up_at, n - 1)
    for m in closing:
        tick(m, 1)
    all_arrived(up_at)
    accumulate(g_up, up_acc)
    gate = gate_acc[...]
    hidden[...] = (gate / (1.0 + jnp.exp(-gate)) * up_acc[...]).astype(jnp.bfloat16)
    eager = g_down.shape[2] == width

    def down_block(j, c):
        place = j * g_down.shape[2] + c * LANES
        p, part = place // width, pl.ds(pl.multiple_of(lax.rem(place, width), LANES), LANES)
        columns = pl.ds(c * LANES, LANES)
        terms = jnp.dot(hidden[...], g_down[j, :, columns], preferred_element_type=f32)
        partial_down[p, :, part] = terms.astype(jnp.bfloat16)
        if eager:
            for d in others:
                @pl.when(j == lax.rem(t + d, tp))
                def _():
                    down_copy(d, c).start()

    for c in range(chunks):
        down_block(f, c)
    for step in range(1, n):
        if step > 1:
            for m in closing:
                tick(m, step)
        for c, m in enumerate(closing):
            def from_way(way, carry):
                j = f + step * (2 * way - 1)

                @pl.when(jnp.logical_and(j >= 0, j < n))
                def _():
                    y_copy(m, way, step).wait_recv()
                    down_block(j, c)

                return carry

            lax.fori_loop(0, 2, from_way, 0)
    if not eager:
        for d in others:
            for c in range(chunks):
                down_copy(d, c).start()
    for d in others:
        for c in range(chunks):
            down_copy(d, c).wait_recv()
    second = partial_down[t].astype(f32)
    for d in others:
        second += heard_down[d - 1].astype(f32)
    second = first_all[t].astype(f32) + second
    ones = jnp.ones((8, width), f32)
    squares[0] = dot(ones, second * second, 1, 1)
    for d in others:
        square_copy(d).start()
    for d in others:
        square_copy(d).wait_recv()
    whole = squares[0]
    for d in others:
        whole += squares[d]
    factor = lax.rsqrt(jnp.transpose(whole) / features + epsilon)[:, :1]
    result_ref[...] = (second * factor * final_gain_ref[...]).astype(jnp.bfloat16)

    for m in range(len(messages)):
        for step in range(1, n):
            for way in (0, 1):
                @pl.when(gives(way, step))
                def _():
                    z_copy(m, way, step).wait_send()

                @pl.when(gets(way, step))
                def _():
                    y_copy(m, way, step).wait_send()
    for d in others:
        for copy in (token_copy, out_copy, first_copy, square_copy):
            copy(d).wait_send()
        for c in range(chunks):
            down_copy(d, c).wait_send()


def body(
    sizes, tokens, attn_gain, w_query, w_key, w_value, w_low, w_lift, decay_bias, head_gain,
    w_out, ffn_gain, w_gate, w_up, w_down, final_gain,
):
    n, tp = sizes
    rows, width = tokens.shape
    bf16, f32 = jnp.bfloat16, jnp.float32
    units, keys, values = w_gate.shape[1], w_query.shape[1], w_value.shape[1]
    mix_width = 2 * keys + values
    held = [pltpu.VMEM((n, w_query.shape[0], mix_width), bf16)]
    held += [pltpu.VMEM((n, *w.shape), bf16) for w in (w_out, w_gate, w_up, w_down)]
    chunks = w_down.shape[1] // LANES
    messages = 6 + chunks
    dma = pltpu.SemaphoreType.DMA
    anywhere = pl.BlockSpec(memory_space=pl.ANY)
    inside = pl.BlockSpec(memory_space=pltpu.VMEM)
    return pl.pallas_call(
        functools.partial(layer_kernel, sizes),
        name="layer",
        out_shape=jax.ShapeDtypeStruct((rows, width), bf16),
        in_specs=[anywhere] + [inside] * 7 + [anywhere] * 7,
        out_specs=inside,
        scratch_shapes=held + [
            pltpu.VMEM((tp, rows, width), bf16),
            pltpu.VMEM((rows, width * tp), bf16),
            pltpu.VMEM((rows, mix_width), bf16),
            pltpu.VMEM((rows, keys), f32),
            pltpu.VMEM((rows, values), bf16),
            pltpu.VMEM((keys // DK, DK, DV), f32),
            pltpu.VMEM((tp, rows, width), bf16),
            pltpu.VMEM((tp - 1, rows, width), bf16),
            pltpu.VMEM((tp, rows, width), bf16),
            pltpu.VMEM((rows, units), f32),
            pltpu.VMEM((rows, units), f32),
            pltpu.VMEM((rows, units), bf16),
            pltpu.VMEM((tp, rows, width), bf16),
            pltpu.VMEM((tp - 1, rows, width), bf16),
            pltpu.VMEM((tp, 8, rows), f32),
            dma((chunks, tp)),
            dma((chunks, tp)),
            dma((messages, 2, n)),
            dma((messages, 2, n)),
            dma((messages, 2, n)),
            dma((messages, 2, n)),
            dma((4, tp)),
            dma((4, tp)),
            dma((8,)),
        ],
        compiler_params=pltpu.CompilerParams(
            collective_id=0, has_side_effects=True, vmem_limit_bytes=63 * 1024 * 1024
        ),
    )(
        tokens, attn_gain[None], w_low.T, w_lift, decay_bias[None], head_gain[None],
        ffn_gain[None], final_gain[None], w_query, w_key, w_value, w_out, w_gate, w_up, w_down,
    )


def solution(mesh):
    sizes = (mesh.shape["fs"], mesh.shape["tp"])
    return jax.shard_map(
        functools.partial(body, sizes),
        mesh=mesh,
        in_specs=(
            P(("grp", "fs"), "tp"),
            P(),
            P("fs", "tp"),
            P("fs", "tp"),
            P("fs", "tp"),
            P(),
            P(None, "tp"),
            P("tp"),
            P(),
            P("tp", "fs"),
            P(),
            P("fs", "tp"),
            P("fs", "tp"),
            P("tp", "fs"),
            P("tp"),
        ),
        out_specs=P(("grp", "fs"), "tp"),
        check_vma=False,
    )
```
